256 devices in a mesh: vp: 32 (over z, x), dp: 8 (over y, core).
Axes of the slice: x: 4, y: 4, z: 8, core: 2. Of those that a mesh axis runs over, the one named last changes fastest.
Arguments:
- stream: bfloat16 [16384, 2048], P(('dp', 'vp')), may hold values from -6 to 6
- norm_gain: float32 [2048], replicated, may hold values from 0.1 to 1.9
- vocab_matrix: bfloat16 [2048, 16384], P(None, 'vp'), may hold values from -0.3125 to 0.3125
- column_bias: float32 [16384], P('vp'), may hold values from -3 to 100
- targets: int32 [16384], P('dp'), may hold values from 0 to 16383
Outputs:
- losses: float32 [16384], P(('dp', 'vp'))
- normin_grad: float32 [16384, 2048], P(('dp', 'vp'))
- vocab_grad: float32 [2048, 16384], P('dp', 'vp')
The draws below stay inside these ranges and needn't reach their ends.
All inputs are finite; a program needn't handle non-finite values.
Results may differ from the reference program's by a relative error of at most 0.0031.
Values may be sent and summed in bfloat16 or wider, within the bound.
No kernel may reach another device: no remote copies, remote signals or barrier semaphores. Data moves between devices by JAX's collectives and lax.ppermute only.
A program may use at most 128 MiB of HBM per device.

```python
import math
import jax
import jax.numpy as jnp
import numpy as np
from jax import lax

D = 2048
V = 16384
TOKENS = 16384
BLOCK_ROWS = 512


def draw_column_bias(key, part):
    columns = jnp.arange(V)
    pattern = 1.2 * jnp.sin(2.3 * (columns * 16 // V).astype(jnp.float32) + 0.4)
    baseline = jnp.clip(jax.random.normal(key, (V,), jnp.float32), -3.0, 3.0) * 0.6
    return baseline + pattern


def plant(array, rng, least, top_value):
    longest = array.shape.index(max(array.shape))
    spots = []
    for shift in (0, 1):
        where = [jax.random.randint(jax.random.fold_in(rng, axis), (), 0, length) for axis, length in enumerate(array.shape)]
        where[longest] = (where[longest] + shift) % array.shape[longest]
        spots.append(tuple(where))
    return array.at[spots[0]].set(least).at[spots[1]].set(top_value)


def level_of(key, shape, cuts, least, largest):
    loudness, own = 1.0, jax.random.fold_in(key, 6)
    for axis_at, shards_of in cuts:
        heights = jnp.exp(jax.random.uniform(jax.random.fold_in(own, axis_at), (shards_of,), jnp.float32, least / len(cuts), largest / len(cuts)))
        loudness = loudness * jnp.repeat(heights, shape[axis_at] // shards_of).reshape([-1 if axis == axis_at else 1 for axis in range(len(shape))])
    return loudness


def rank_bounds(amount, slope):
    loads = [(1 << 20) // math.isqrt(standing ** slope) + 1 for standing in range(1, amount + 1)]
    spread = 1 + sum(loads) // (1 << 30)
    return np.cumsum(np.array([max(1, weight // spread) for weight in loads]))


def skewed_ids(key, shape, number_of, skew):
    grid = rank_bounds(number_of, skew)
    lot = jax.random.randint(jax.random.fold_in(key, 1), shape, 0, int(grid[number_of - 1]))
    grade = jnp.searchsorted(jnp.asarray(grid, jnp.int32), lot, side="right")
    return jax.random.permutation(jax.random.fold_in(key, 2), number_of)[grade].astype(jnp.int32)


def bell_draw(rng, extent, scale, reach, pieces=(), kind=jnp.bfloat16):
    loudness = level_of(rng, extent, pieces, -0.22, 0.18) if pieces else 1.0
    result = jax.random.normal(rng, extent, jnp.float32) * scale * loudness
    return jnp.minimum(jnp.maximum(result, -reach), reach).astype(kind)


def setup_inputs(seed: int = 0) -> dict:
    keys = jax.random.split(jax.random.key(seed), 6)
    return {
        "stream": bell_draw(keys[0], (TOKENS, D), 1.0, 6.0, ((0, 256),)),
        "norm_gain": jnp.clip(1.0 + 0.18 * jax.random.normal(keys[1], (D,), jnp.float32), 0.1, 1.9),
        "vocab_matrix": bell_draw(keys[2], (D, V), (D // 6) ** -0.5, 0.3125, ((1, 32),)),
        "column_bias": draw_column_bias(jax.random.fold_in(keys[5], 71), 0),
        "targets": plant(skewed_ids(keys[4], (TOKENS,), V, 2), jax.random.fold_in(keys[4], 3), 0, V - 1).astype(jnp.int32),
    }


PENALTY = 0.001
EPSILON = 1e-06

def reference(stream, norm_gain, vocab_matrix, column_bias, targets):
    normin = stream.astype(jnp.float32)
    inverse = lax.rsqrt(lax.optimization_barrier(jnp.mean(normin * normin, axis=1, keepdims=True)) + EPSILON)
    normed = (normin * inverse * norm_gain).astype(jnp.bfloat16)
    num_blocks = TOKENS // BLOCK_ROWS
    columns = jnp.arange(vocab_matrix.shape[1], dtype=jnp.int32)

    def advance(running, block_index):
        start_row = (block_index * BLOCK_ROWS).astype(jnp.int32)
        block_normed = lax.dynamic_slice_in_dim(normed, start_row, BLOCK_ROWS, 0)
        wanted = lax.dynamic_slice_in_dim(targets, start_row, BLOCK_ROWS, 0)
        scores = jnp.dot(block_normed, vocab_matrix, preferred_element_type=jnp.float32) + column_bias
        row_max = lax.optimization_barrier(jnp.max(scores, axis=1, keepdims=True))
        row_sum = lax.optimization_barrier(jnp.sum(jnp.exp(scores - row_max), axis=1, keepdims=True))
        log_total = row_max + jnp.log(row_sum)
        is_target = columns[None, :] == wanted[:, None]
        picked = lax.optimization_barrier(jnp.sum(jnp.where(is_target, scores, 0.0), axis=1))
        flat_total = log_total[:, 0]
        block_loss = flat_total - picked + PENALTY * flat_total * flat_total
        factor = 1.0 + 2.0 * PENALTY * log_total
        weight = (jnp.exp(scores - log_total) * factor - is_target.astype(jnp.float32)).astype(jnp.bfloat16)
        rows_grad = lax.dot_general(weight, vocab_matrix, (((1,), (1,)), ((), ())), preferred_element_type=jnp.float32)
        running = running + lax.dot_general(block_normed, weight, (((0,), (0,)), ((), ())), preferred_element_type=jnp.float32)
        return (running, (block_loss, rows_grad))
    zeros_grad = jnp.zeros((vocab_matrix.shape[0], vocab_matrix.shape[1]), jnp.float32)
    vocab_grad, (losses, rows_grad) = lax.scan(advance, zeros_grad, jnp.arange(num_blocks, dtype=jnp.int32))
    losses = losses.reshape(-1)
    rows_grad = rows_grad.reshape(-1, vocab_matrix.shape[0])
    scaled = rows_grad * norm_gain
    projected = lax.optimization_barrier(jnp.mean(scaled * normin, axis=1, keepdims=True))
    normin_grad = inverse * (scaled - normin * inverse * inverse * projected)
    return (losses, normin_grad, vocab_grad)
```

```python
import jax
import jax.numpy as jnp
from jax import lax
from jax.sharding import Mesh
from jax.sharding import PartitionSpec as P

PENALTY = 0.001
EPSILON = 1e-06
BF16 = jnp.bfloat16
F32 = jnp.float32
VP = ("z", "x")
DP = ("y", "c")


def shift(value, axis, step):
    size = lax.axis_size(axis)
    return lax.ppermute(value, axis, [(i, (i + step) % size) for i in range(size)])


def mirrored(value, axis):
    size = lax.axis_size(axis)
    flipped = jnp.flip(value, 0)
    start = size - 1 - lax.axis_index(axis)
    return lax.dynamic_slice_in_dim(jnp.concatenate([flipped, flipped]), start, size, 0)


def relative(value):
    value = mirrored(value, "z")
    return jnp.swapaxes(mirrored(jnp.swapaxes(value, 0, 1), "x"), 0, 1)


def gather_line(own, axis):
    size = lax.axis_size(axis)
    found = [None] * size
    found[0] = up = down = own
    for step in range(1, size // 2):
        up = shift(up, axis, 1)
        down = shift(down, axis, -1)
        found[step] = up
        found[size - step] = down
    half = own.shape[0] // 2
    found[size // 2] = jnp.concatenate(
        [shift(up[:half], axis, 1), shift(down[half:], axis, -1)]
    )
    return found


def scatter_line(part, axis, dtype):
    size = lax.axis_size(axis)
    middle = size // 2
    both = slice(None)
    rows = part(0, both).shape[0]
    low, high = slice(0, rows // 2), slice(rows // 2, rows)
    up = shift(part(middle, low).astype(dtype), axis, 1).astype(F32)
    down = shift(part(middle, high).astype(dtype), axis, -1).astype(F32)
    up = jnp.pad(up, ((0, rows - rows // 2), (0, 0)))
    down = jnp.pad(down, ((rows // 2, 0), (0, 0)))
    for step in range(1, middle):
        up = shift((part(middle + step, both) + up).astype(dtype), axis, 1).astype(F32)
        down = shift((part(middle - step, both) + down).astype(dtype), axis, -1).astype(F32)
    return part(0, both) + up + down


def per_device(stream, norm_gain, vocab_matrix, column_bias, targets):
    zs, xs = lax.axis_size("z"), lax.axis_size("x")
    my_rows, width = stream.shape
    cols = vocab_matrix.shape[1]
    half = my_rows // 2
    shard = lax.axis_index("z") * xs + lax.axis_index("x")

    normin = stream.astype(F32)
    inverse = lax.rsqrt(jnp.mean(normin * normin, axis=1, keepdims=True) + EPSILON)
    normed = (normin * inverse * norm_gain).astype(BF16)

    chunks_a = gather_line(jnp.concatenate(gather_line(normed[:half], "x")), "z")
    chunks_b = gather_line(jnp.concatenate(gather_line(normed[half:], "z")), "x")

    wanted = relative((targets - shard * cols).reshape(zs, xs, my_rows))
    wanted_a = wanted[:, :, :half].reshape(zs, xs * half)
    wanted_b = jnp.swapaxes(wanted[:, :, half:], 0, 1).reshape(xs, zs * half)
    columns = jnp.arange(cols, dtype=jnp.int32)

    chunks = chunks_a + chunks_b
    goals = [wanted_a[k] for k in range(zs)] + [wanted_b[k] for k in range(xs)]
    scores, spans, picks = [], [], []
    for chunk, goal in zip(chunks, goals):
        score = jnp.dot(chunk, vocab_matrix, preferred_element_type=F32) + column_bias
        top = jnp.max(score, axis=1)
        spans.append(top + jnp.log(jnp.sum(jnp.exp(score - top[:, None]), axis=1)))
        hit = columns[None, :] == goal[:, None]
        picks.append(jnp.sum(jnp.where(hit, score, 0.0), axis=1))
        scores.append(score)

    def by_owner(parts):
        first = jnp.stack(parts[:zs]).reshape(zs, xs, half)
        second = jnp.swapaxes(jnp.stack(parts[zs:]).reshape(xs, zs, half), 0, 1)
        return relative(jnp.concatenate([first, second], axis=2))

    devices = zs * xs
    span = by_owner(spans).reshape(1, -1, 128)
    pick = jnp.pad(by_owner(picks).reshape(devices, 1, my_rows), ((0, 0), (0, 0), (0, 128 - my_rows)))
    sent = jnp.concatenate([jnp.broadcast_to(span, (devices, *span.shape[1:])), pick], axis=1)
    got = lax.all_to_all(sent, VP, 0, 0, tiled=True)
    spans_all = got[:, :-1].reshape(devices, -1)
    top = jnp.max(spans_all, axis=0)
    log_total = top + jnp.log(jnp.sum(jnp.exp(spans_all - top), axis=0))
    picked = jnp.sum(got[:, -1, :my_rows], axis=0)
    own_total = lax.dynamic_slice_in_dim(log_total, shard * my_rows, my_rows, 0)
    losses = own_total - picked + PENALTY * own_total * own_total

    totals = relative(log_total.reshape(zs, xs, my_rows))
    totals_a = totals[:, :, :half].reshape(zs, xs * half)
    totals_b = jnp.swapaxes(totals[:, :, half:], 0, 1).reshape(xs, zs * half)
    totals = [totals_a[k] for k in range(zs)] + [totals_b[k] for k in range(xs)]
    weights = []
    for score, goal, total in zip(scores, goals, totals):
        hit = columns[None, :] == goal[:, None]
        factor = 1.0 + 2.0 * PENALTY * total[:, None]
        weights.append(
            (jnp.exp(score - total[:, None]) * factor - hit.astype(F32)).astype(BF16)
        )

    def rows_of(weight):
        return lax.dot_general(
            weight, vocab_matrix, (((1,), (1,)), ((), ())), preferred_element_type=F32
        )

    sum_a = scatter_line(lambda k, rows: rows_of(weights[k][rows]), "z", BF16)
    sum_b = scatter_line(lambda k, rows: rows_of(weights[zs + k][rows]), "x", BF16)
    sum_a = sum_a.reshape(xs, half, width)
    sum_b = sum_b.reshape(zs, half, width)
    rows_a = scatter_line(lambda k, rows: sum_a[k][rows], "x", F32)
    rows_b = scatter_line(lambda k, rows: sum_b[k][rows], "z", F32)
    rows_grad = jnp.concatenate([rows_a, rows_b])

    local_grad = lax.dot_general(
        jnp.concatenate(chunks),
        jnp.concatenate(weights),
        (((0,), (0,)), ((), ())),
        preferred_element_type=F32,
    ).astype(BF16)
    owners = lax.axis_size(DP)
    parts = local_grad.reshape(owners, width // owners, cols)
    arrived = lax.all_to_all(parts, DP, 0, 0, tiled=True)
    vocab_grad = jnp.sum(arrived.astype(F32), axis=0)

    scaled = rows_grad * norm_gain
    projected = jnp.mean(scaled * normin, axis=1, keepdims=True)
    normin_grad = inverse * (scaled - normin * inverse * inverse * projected)
    return (losses, normin_grad, vocab_grad)


def solution(mesh):
    torus = Mesh(mesh.devices.reshape(8, 4, 4, 2), ("z", "x", "y", "c"))
    everyone = DP + VP
    in_specs = (P(everyone, None), P(), P(None, VP), P(VP), P(DP))
    out_specs = (P(everyone), P(everyone, None), P(DP, VP))
    return jax.shard_map(
        per_device, mesh=torus, in_specs=in_specs, out_specs=out_specs, check_vma=False
    )
```

```python
import jax
import jax.numpy as jnp
from jax import lax
from jax.sharding import Mesh
from jax.sharding import PartitionSpec as P

PENALTY = 0.001
EPSILON = 1e-06
BF16 = jnp.bfloat16
F32 = jnp.float32
X = ("xp", "xm")
VP = ("z", *X)
DP = ("y", "c")
GROUP = ("c", "z", "xm")


def shift(value, axis, step):
    size = lax.axis_size(axis)
    return lax.ppermute(value, axis, [(i, (i + step) % size) for i in range(size)])


def mirrored(value, axis, dim):
    size = lax.axis_size(axis)
    flipped = jnp.flip(value, dim)
    start = size - 1 - lax.axis_index(axis)
    return lax.dynamic_slice_in_dim(jnp.concatenate([flipped, flipped], dim), start, size, dim)


def relative(value):
    for dim, axis in enumerate(GROUP):
        value = mirrored(value, axis, dim)
    return value


def gather_ring(own):
    size = lax.axis_size("z")
    found = [None] * size
    found[0] = up = down = own
    for step in range(1, size // 2):
        up, down = shift(up, "z", 1), shift(down, "z", -1)
        up, down = lax.optimization_barrier((up, down))
        found[step] = up
        found[size - step] = down
    half = own.shape[0] // 2
    found[size // 2] = jnp.concatenate([shift(up[:half], "z", 1), shift(down[half:], "z", -1)])
    return found


def scatter_ring(part):
    middle = lax.axis_size("z") // 2
    both = slice(None)
    rows = 2 * part(middle, slice(0, 8)).shape[0] if False else part(0, both).shape[0]
    low, high = slice(0, rows // 2), slice(rows // 2, rows)
    up = shift(part(middle, low).astype(BF16), "z", 1).astype(F32)
    down = shift(part(middle, high).astype(BF16), "z", -1).astype(F32)
    up = jnp.pad(up, ((0, rows // 2), (0, 0)))
    down = jnp.pad(down, ((rows // 2, 0), (0, 0)))
    for step in range(1, middle):
        up = shift((part(middle + step, both) + up).astype(BF16), "z", 1)
        down = shift((part(middle - step, both) + down).astype(BF16), "z", -1)
        up, down = lax.optimization_barrier((up, down))
        up, down = up.astype(F32), down.astype(F32)
    return part(0, both) + up + down


def per_device(stream, norm_gain, vocab_matrix, column_bias, targets):
    zs, xs = lax.axis_size("z"), 4
    my_rows, width = stream.shape
    cols = vocab_matrix.shape[1]
    xp, xm, core = lax.axis_index("xp"), lax.axis_index("xm"), lax.axis_index("c")
    x = 2 * xp + xm

    across = [(2 * i, 2 * i) for i in range(xs)] + [(2 * i + 1, 2 * (3 - i) + 1) for i in range(xs)]
    vocab = lax.ppermute(vocab_matrix, (*X, "c"), across)
    bias = lax.ppermute(column_bias, (*X, "c"), across)
    shard = lax.axis_index("z") * xs + jnp.where(core == 0, x, 3 - x)

    normin = stream.astype(F32)
    inverse = lax.rsqrt(jnp.mean(normin * normin, axis=1, keepdims=True) + EPSILON)
    normed = (normin * inverse * norm_gain).astype(BF16)

    pair = jnp.concatenate([normed, shift(normed, "xm", 1)])
    mine = gather_ring(pair)
    theirs = [shift(chunk, "c", 1) for chunk in mine]

    my_goals = lax.dynamic_slice_in_dim(targets.reshape(zs, xs, my_rows), 2 * xp, 2, 1)
    goals = jnp.stack([my_goals, shift(my_goals, "c", 1)]) - shard * cols
    goals = mirrored(mirrored(goals, "z", 1), "xm", 2).reshape(2, zs, 2 * my_rows)
    columns = jnp.arange(cols, dtype=jnp.int32)

    scores, spans, picks = [], [], []
    for side, chunks in enumerate((mine, theirs)):
        for k, chunk in enumerate(chunks):
            score = jnp.dot(chunk, vocab, preferred_element_type=F32) + bias
            top = jnp.max(score, axis=1)
            spans.append(top + jnp.log(jnp.sum(jnp.exp(score - top[:, None]), axis=1)))
            hit = columns[None, :] == goals[side, k][:, None]
            picks.append(jnp.sum(jnp.where(hit, score, 0.0), axis=1))
            scores.append(score)

    devices = 4 * zs
    shape = (2, zs, 2, my_rows)
    span = relative(jnp.stack(spans).reshape(shape)).reshape(1, -1, 128)
    pick = relative(jnp.stack(picks).reshape(shape)).reshape(devices, 1, my_rows)
    pick = jnp.pad(pick, ((0, 0), (0, 0), (0, 128 - my_rows)))
    sent = jnp.concatenate([jnp.broadcast_to(span, (devices, *span.shape[1:])), pick], axis=1)
    got = lax.all_to_all(sent, GROUP, 0, 0, tiled=True)
    spans_all = got[:, :-1].reshape(devices, -1)
    top = jnp.max(spans_all, axis=0)
    log_total = top + jnp.log(jnp.sum(jnp.exp(spans_all - top), axis=0))
    picked = jnp.sum(got[:, -1, :my_rows], axis=0)
    place = lax.axis_index(GROUP)
    own_total = lax.dynamic_slice_in_dim(log_total, place * my_rows, my_rows, 0)
    losses = own_total - picked + PENALTY * own_total * own_total

    totals = relative(log_total.reshape(shape)).reshape(2, zs, 2 * my_rows)
    weights = []
    for side in range(2):
        for k in range(zs):
            hit = columns[None, :] == goals[side, k][:, None]
            total = totals[side, k][:, None]
            factor = 1.0 + 2.0 * PENALTY * total
            raised = jnp.exp(scores[side * zs + k] - total)
            weights.append((raised * factor - hit.astype(F32)).astype(BF16))

    def rows_of(weight):
        return lax.dot_general(
            weight, vocab, (((1,), (1,)), ((), ())), preferred_element_type=F32
        )

    crossed = [shift(rows_of(weight).astype(BF16), "c", 1) for weight in weights[zs:]]
    pair_sum = scatter_ring(lambda k, rows: rows_of(weights[k][rows]) + crossed[k][rows].astype(F32))
    beside = shift(pair_sum[my_rows:].astype(BF16), "xm", 1)
    rows_grad = pair_sum[:my_rows] + beside.astype(F32)

    local_grad = lax.dot_general(
        jnp.concatenate(mine + theirs),
        jnp.concatenate(weights),
        (((0,), (0,)), ((), ())),
        preferred_element_type=F32,
    ).astype(BF16)
    ys = lax.axis_size("y")
    parts = local_grad.reshape(ys, width // ys, cols)
    arrived = lax.all_to_all(parts, "y", 0, 0, tiled=True)
    blocks = jnp.sum(arrived.astype(F32), axis=0).reshape(2, -1, cols)
    home = [(2 * i, 2 * i + 1) for i in range(xs)] + [(2 * i + 1, 2 * (3 - i)) for i in range(xs)]
    first = lax.dynamic_slice_in_dim(blocks, 1 - core, 1, 0)[0]
    second = lax.dynamic_slice_in_dim(blocks, core, 1, 0)[0]
    vocab_grad = lax.ppermute(first, (*X, "c"), home) + lax.ppermute(second, (*X, "c"), across)

    scaled = rows_grad * norm_gain
    projected = jnp.mean(scaled * normin, axis=1, keepdims=True)
    normin_grad = inverse * (scaled - normin * inverse * inverse * projected)
    return (losses, normin_grad, vocab_grad)


def solution(mesh):
    torus = Mesh(mesh.devices.reshape(8, 2, 2, 4, 2), ("z", "xp", "xm", "y", "c"))
    everyone = DP + VP
    in_specs = (P(everyone, None), P(), P(None, VP), P(VP), P(DP))
    out_specs = (P(everyone), P(everyone, None), P(DP, VP))
    return jax.shard_map(
        per_device, mesh=torus, in_specs=in_specs, out_specs=out_specs, check_vma=False
    )
```

```python
import jax
import jax.numpy as jnp
from jax import lax
from jax.experimental import pallas as pl
from jax.experimental.pallas import tpu as pltpu
from jax.sharding import Mesh
from jax.sharding import PartitionSpec as P

PENALTY = 0.001
EPSILON = 1e-06
BF16 = jnp.bfloat16
F32 = jnp.float32
X = ("xp", "xm")
VP = ("z", *X)
DP = ("y", "c")
GROUP = ("c", "z", "xm")


def shift(value, axis, step):
    size = lax.axis_size(axis)
    return lax.ppermute(value, axis, [(i, (i + step) % size) for i in range(size)])


def mirrored(value, axis, dim):
    size = lax.axis_size(axis)
    flipped = jnp.flip(value, dim)
    start = size - 1 - lax.axis_index(axis)
    return lax.dynamic_slice_in_dim(jnp.concatenate([flipped, flipped], dim), start, size, dim)


def turned(row, place):
    return jnp.where(place[2] == 1, pltpu.roll(row, row.shape[1] // 2, 1), row)


def pack_kernel(place, tops, sums, picks, sent, spans, hits):
    sides, zs = tops.shape[:2]
    spans[...] = tops[...] + jnp.log(sums[...])
    for side in range(sides):
        for z in range(zs):
            line = (place[0] ^ side, pl.ds((place[1] + zs - z) % zs, 1))
            span, hit = turned(spans[line], place), turned(picks[line], place)
            at = side * zs + z
            hits[at : at + 1, :] = span
            sent[2 * at, sides * zs :, :] = hit
            sent[2 * at + 1, sides * zs :, :] = pltpu.roll(hit, hit.shape[1] // 2, 1)
    everyone = hits[...]
    for device in range(sent.shape[0]):
        sent[device, : sides * zs, :] = everyone


def unpack_kernel(place, got, totals, losses, held):
    sides, zs = totals.shape[:2]
    spans = got[:, : sides * zs, :]
    top = jnp.max(spans, axis=0)
    held[...] = top + jnp.log(jnp.sum(jnp.exp(spans - top[None]), axis=0))
    for side in range(sides):
        for k in range(zs):
            row = (place[0] ^ side) * zs + (place[1] + zs - k) % zs
            totals[side, k : k + 1, :] = turned(held[pl.ds(row, 1), :], place)
    own = turned(held[pl.ds(place[0] * zs + place[1], 1), :], place)
    picked = jnp.sum(got[:, sides * zs :, :], axis=0)
    losses[...] = own - picked + PENALTY * own * own


def small_call(kernel, place, arrays, shapes, scratch):
    vmem = pl.BlockSpec(memory_space=pltpu.VMEM)
    smem = pl.BlockSpec(memory_space=pltpu.SMEM)
    return pl.pallas_call(
        kernel,
        in_specs=[smem] + [vmem] * len(arrays),
        out_specs=[vmem] * len(shapes),
        out_shape=[jax.ShapeDtypeStruct(shape, F32) for shape in shapes],
        scratch_shapes=[pltpu.VMEM(shape, F32) for shape in scratch],
        compiler_params=pltpu.CompilerParams(vmem_limit_bytes=4 << 20),
    )(place, *arrays)


def score_of(chunk, vocab, bias, goal):
    score = jnp.dot(chunk, vocab, preferred_element_type=F32) + bias
    top = jnp.max(score, axis=1)
    total = jnp.sum(jnp.exp(score - top[:, None]), axis=1)
    columns = jnp.arange(vocab.shape[1], dtype=jnp.int32)
    pick = jnp.sum(jnp.where(columns[None, :] == goal[:, None], score, 0.0), axis=1)
    return score, top, total, pick


def weight_of(score, goal, log_total):
    factor = 1.0 + 2.0 * PENALTY * log_total
    columns = lax.broadcasted_iota(jnp.int32, score.shape, 1)
    hit = (columns == goal).astype(F32)
    return (jnp.exp(score - log_total) * factor - hit).astype(BF16)


def per_device(stream, norm_gain, vocab_matrix, column_bias, targets):
    zs, xs = lax.axis_size("z"), 4
    mid = zs // 2
    my_rows, width = stream.shape
    cols = vocab_matrix.shape[1]
    xp, xm, core = lax.axis_index("xp"), lax.axis_index("xm"), lax.axis_index("c")
    x = 2 * xp + xm

    normin = stream.astype(F32)
    inverse = lax.rsqrt(jnp.mean(normin * normin, axis=1, keepdims=True) + EPSILON)
    normed = (normin * inverse * norm_gain).astype(BF16)

    pair = jnp.concatenate([normed, shift(normed, "xm", 1)])
    vocab_matrix, _ = lax.optimization_barrier((vocab_matrix, normed))
    across = [(2 * i, 2 * i) for i in range(xs)] + [(2 * i + 1, 2 * (3 - i) + 1) for i in range(xs)]
    vocab = lax.ppermute(vocab_matrix, (*X, "c"), across)
    bias = lax.ppermute(column_bias, (*X, "c"), across)
    shard = lax.axis_index("z") * xs + jnp.where(core == 0, x, 3 - x)

    my_goals = lax.dynamic_slice_in_dim(targets.reshape(zs, xs, my_rows), 2 * xp, 2, 1)
    goals = jnp.stack([my_goals, shift(my_goals, "c", 1)]) - shard * cols
    goals = mirrored(mirrored(goals, "z", 1), "xm", 2).reshape(2, zs, 2 * my_rows)

    chunks, scored = {}, {}

    lines = jnp.zeros((4 * zs * my_rows, width), BF16)

    def arrive(distance, chunk, half=None):
        chunks[0, distance, half] = chunk
        chunks[1, distance, half] = shift(chunk, "c", 1)

    scores = jnp.zeros((4 * zs * my_rows, cols), F32)

    def row_of(key):
        return (2 * (key[0] * zs + key[1]) + (key[2] or 0)) * my_rows

    def lay(lines, keys):
        for key in keys:
            lines = lax.dynamic_update_slice_in_dim(lines, chunks[key], row_of(key), 0)
        return lines

    def goal_of(key):
        goal = goals[key[0], key[1]]
        return goal if key[2] is None else goal[key[2] * my_rows : (key[2] + 1) * my_rows]

    def score_now(scores, keys):
        for key in keys:
            score, *scored[key] = score_of(chunks[key], vocab, bias, goal_of(key))
            scores = lax.dynamic_update_slice_in_dim(scores, score, row_of(key), 0)
        return scores

    def keys_at(*distances):
        return [key for distance in distances for key in chunks if key[1] == distance]

    arrive(0, pair)
    up = down = pair
    held = []
    for step in range(1, mid):
        up, down = shift(up, "z", 1), shift(down, "z", -1)
        if step >= 2:
            held = keys_at(*{step - 2, (2 - step) % zs})
            scores = score_now(scores, held)
            lines = lay(lines, held)
        up, down, lines, scores, kept = lax.optimization_barrier(
            (up, down, lines, scores, [scored[key] for key in held])
        )
        scored.update(zip(held, kept))
        arrive(step, up)
        arrive(zs - step, down)
    low, high = shift(up[:my_rows], "z", 1), shift(down[my_rows:], "z", -1)
    held = keys_at(mid - 2, zs - mid + 2)
    scores = score_now(scores, held)
    lines = lay(lines, held)
    low, high, lines, scores, kept = lax.optimization_barrier(
        (low, high, lines, scores, [scored[key] for key in held])
    )
    scored.update(zip(held, kept))
    arrive(mid, low, 0)
    arrive(mid, high, 1)
    held = keys_at(mid - 1, zs - mid + 1, mid)
    scores = score_now(scores, held)
    lines = lay(lines, held)

    order = [(side, k, half) for side in range(2) for k in range(zs) for half in (None, 0, 1)]
    order = [key for key in order if key in chunks]

    def by_distance(part):
        return jnp.concatenate([scored[key][part] for key in order]).reshape(2, zs, 2 * my_rows)

    devices = 4 * zs
    lines_of = (2, zs, 2 * my_rows)
    place = jnp.stack([core, lax.axis_index("z"), xm]).astype(jnp.int32)
    (sent,) = small_call(
        pack_kernel,
        place,
        [by_distance(part) for part in (0, 1, 2)],
        [(devices, 2 * zs + 1, 2 * my_rows)],
        [lines_of, (2 * zs, 2 * my_rows)],
    )
    got = lax.all_to_all(sent, GROUP, 0, 0, tiled=True)
    totals, losses = small_call(
        unpack_kernel, place, [got], [lines_of, (1, 2 * my_rows)], [(2 * zs, 2 * my_rows)]
    )
    losses = losses[0, :my_rows]
    weights = weight_of(scores, goals.reshape(-1, 1), totals.reshape(-1, 1))

    def rows_of(key, weights):
        row, count = row_of(key), chunks[key].shape[0]
        return lax.dot_general(
            weights[row : row + count],
            vocab,
            (((1,), (1,)), ((), ())),
            preferred_element_type=F32,
        )

    def both_cores(distance, weights, half=None):
        part = rows_of((1, distance, half), weights)
        crossed = shift(part, "c", 1)
        return lambda: rows_of((0, distance, half), weights) + crossed

    up = both_cores(mid, weights, 0)().astype(BF16)
    down = both_cores(mid, weights, 1)().astype(BF16)
    up, down, weights = lax.optimization_barrier((up, down, weights))
    up, down = shift(up, "z", 1), shift(down, "z", -1)
    up, down = up.astype(F32), down.astype(F32)
    up = jnp.pad(up, ((0, my_rows), (0, 0)))
    down = jnp.pad(down, ((my_rows, 0), (0, 0)))
    for step in range(1, mid):
        ahead = both_cores(mid + step, weights)
        behind = both_cores(mid - step, weights)
        up, down = (ahead() + up).astype(BF16), (behind() + down).astype(BF16)
        up, down, weights = lax.optimization_barrier((up, down, weights))
        up, down = shift(up, "z", 1), shift(down, "z", -1)
        if step == 1:
            local_grad = lax.dot_general(
                lines, weights, (((0,), (0,)), ((), ())), preferred_element_type=F32
            ).astype(BF16)
            up, down, local_grad = lax.optimization_barrier((up, down, local_grad))
        up, down = lax.optimization_barrier((up, down))
        up, down = up.astype(F32), down.astype(F32)
    pair_sum = both_cores(0, weights)() + up + down
    beside = shift(pair_sum[my_rows:].astype(BF16), "xm", 1)
    rows_grad = pair_sum[:my_rows] + beside.astype(F32)

    ys = lax.axis_size("y")
    parts = local_grad.reshape(ys, width // ys, cols)
    arrived = lax.all_to_all(parts, "y", 0, 0, tiled=True)
    blocks = jnp.sum(arrived.astype(F32), axis=0).reshape(2, -1, cols)
    home = [(2 * i, 2 * i + 1) for i in range(xs)] + [(2 * i + 1, 2 * (3 - i)) for i in range(xs)]
    first = lax.dynamic_slice_in_dim(blocks, 1 - core, 1, 0)[0]
    second = lax.dynamic_slice_in_dim(blocks, core, 1, 0)[0]
    vocab_grad = lax.ppermute(first, (*X, "c"), home) + lax.ppermute(second, (*X, "c"), across)

    scaled = rows_grad * norm_gain
    projected = jnp.mean(scaled * normin, axis=1, keepdims=True)
    normin_grad = inverse * (scaled - normin * inverse * inverse * projected)
    return (losses, normin_grad, vocab_grad)


def solution(mesh):
    torus = Mesh(mesh.devices.reshape(8, 2, 2, 4, 2), ("z", "xp", "xm", "y", "c"))
    everyone = DP + VP
    in_specs = (P(everyone, None), P(), P(None, VP), P(VP), P(DP))
    out_specs = (P(everyone), P(everyone, None), P(DP, VP))

    return jax.shard_map(
        per_device, mesh=torus, in_specs=in_specs, out_specs=out_specs, check_vma=False
    )
```

```python
import functools

import jax
import jax.numpy as jnp
from jax import lax
from jax.experimental import pallas as pl
from jax.experimental.pallas import tpu as pltpu
from jax.sharding import Mesh
from jax.sharding import PartitionSpec as P

PENALTY = 0.001
EPSILON = 1e-06
BF16 = jnp.bfloat16
F32 = jnp.float32
X = ("xp", "xm")
VP = ("z", *X)
DP = ("y", "c")
GROUP = ("c", "z", "xm")
LANES = 128
ANY = pl.BlockSpec(memory_space=pl.ANY)
HBM = pl.BlockSpec(memory_space=pltpu.HBM)
VMEM = pl.BlockSpec(memory_space=pltpu.VMEM)
SMEM = pl.BlockSpec(memory_space=pltpu.SMEM)


def shift(value, axis, step):
    size = lax.axis_size(axis)
    return lax.ppermute(value, axis, [(i, (i + step) % size) for i in range(size)])


def mirrored(value, axis, dim):
    size = lax.axis_size(axis)
    flipped = jnp.flip(value, dim)
    start = size - 1 - lax.axis_index(axis)
    return lax.dynamic_slice_in_dim(jnp.concatenate([flipped, flipped], dim), start, size, dim)


def turned(row, place):
    return jnp.where(place[2] == 1, pltpu.roll(row, row.shape[1] // 2, 1), row)


def score_kernel(n, first, *refs):
    chunks, (vocab, bias, goals) = refs[:n], refs[n : n + 3]
    lines, scores, stats, x_buf, s_buf, sems = refs[-6:]
    rows = x_buf.shape[0]
    copies, row = [], 0
    for i, chunk in enumerate(chunks):
        place = x_buf.at[pl.ds(row, chunk.shape[0])]
        copies.append(pltpu.make_async_copy(chunk, place, sems.at[i]))
        row += chunk.shape[0]
    for copy in copies:
        copy.start()
    for copy in copies:
        copy.wait()
    out_x = pltpu.make_async_copy(x_buf, lines.at[pl.ds(first, rows)], sems.at[n])
    out_x.start()
    s_buf[...] = jnp.dot(x_buf[...], vocab[...], preferred_element_type=F32) + bias[...]
    out_s = pltpu.make_async_copy(s_buf, scores.at[pl.ds(first, rows)], sems.at[n + 1])
    out_s.start()
    diagonal = lax.broadcasted_iota(jnp.int32, (LANES, LANES), 0) == lax.broadcasted_iota(
        jnp.int32, (LANES, LANES), 1
    )

    def across(column):
        return jnp.sum(jnp.where(diagonal, column, 0.0), axis=0, keepdims=True)

    for g in range(rows // LANES):
        at = pl.ds(g * LANES, LANES)
        score = s_buf[at, :]
        top = jnp.max(score, axis=1, keepdims=True)
        total = jnp.sum(jnp.exp(score - top), axis=1, keepdims=True)
        hit = lax.broadcasted_iota(jnp.int32, score.shape, 1) == goals[at, :]
        pick = jnp.sum(jnp.where(hit, score, 0.0), axis=1, keepdims=True)
        stats[0, g : g + 1, :] = across(top + jnp.log(total))
        stats[1, g : g + 1, :] = across(pick)
    out_x.wait()
    out_s.wait()


def score_stage(chunks, vocab, bias, goals, first, held):
    rows = sum(chunk.shape[0] for chunk in chunks)
    n, (width, cols), every = len(chunks), vocab.shape, goals.shape[0]
    goal_block = pl.BlockSpec((rows, 1), lambda: (0, 0))
    return pl.pallas_call(
        functools.partial(score_kernel, n, first),
        in_specs=[ANY] * n + [VMEM, VMEM, goal_block] + [HBM, ANY][: len(held)],
        out_specs=[HBM, ANY, VMEM],
        out_shape=[
            pltpu.HBM((every, width), BF16),
            pltpu.HBM((every, cols), F32),
            jax.ShapeDtypeStruct((2, rows // LANES, LANES), F32),
        ],
        scratch_shapes=[
            pltpu.VMEM((rows, width), BF16),
            pltpu.VMEM((rows, cols), F32),
            pltpu.SemaphoreType.DMA((n + 2,)),
        ],
        input_output_aliases={n + 3 + i: i for i in range(len(held))},
        compiler_params=pltpu.CompilerParams(vmem_limit_bytes=14 << 20),
        cost_estimate=pl.CostEstimate(
            flops=2 * rows * width * cols, transcendentals=rows * cols, bytes_accessed=8 << 20
        ),
        name="score",
    )(*chunks, vocab, bias, lax.slice_in_dim(goals, first, first + rows, axis=0), *held)


def stage_rows(zs):
    found = []
    for step in range(zs // 2 + 1):
        distances = sorted({step, (zs - step) % zs})
        found += [(side, k) for side in range(2) for k in distances]
    return found


def pack_kernel(n, place, *refs):
    stats, (sent, spans, hits, joined) = refs[:n], refs[n:]
    zs = spans.shape[1]
    order, group = stage_rows(zs), 0
    for stat in stats:
        for g in range(stat.shape[1]):
            side, k = order[group]
            spans[side, k : k + 1, :] = stat[0, g : g + 1, :]
            hits[side, k : k + 1, :] = stat[1, g : g + 1, :]
            group += 1
    for side in range(2):
        for z in range(zs):
            line = (place[0] ^ side, pl.ds((place[1] + zs - z) % zs, 1))
            span, hit = turned(spans[line], place), turned(hits[line], place)
            at = side * zs + z
            joined[at : at + 1, :] = span
            sent[2 * at, 2 * zs :, :] = hit
            sent[2 * at + 1, 2 * zs :, :] = pltpu.roll(hit, hit.shape[1] // 2, 1)
    everyone = joined[...]
    for device in range(sent.shape[0]):
        sent[device, : 2 * zs, :] = everyone


def unpack_kernel(place, got, totals, losses, held):
    zs = held.shape[0] // 2
    spans = got[:, : 2 * zs, :]
    top = jnp.max(spans, axis=0)
    held[...] = top + jnp.log(jnp.sum(jnp.exp(spans - top[None]), axis=0))
    for group, (side, k) in enumerate(stage_rows(zs)):
        row = (place[0] ^ side) * zs + (place[1] + zs - k) % zs
        totals[group : group + 1, :] = turned(held[pl.ds(row, 1), :], place)
    own = turned(held[pl.ds(place[0] * zs + place[1], 1), :], place)
    picked = jnp.sum(got[:, 2 * zs :, :], axis=0)
    losses[...] = own - picked + PENALTY * own * own


def small_call(kernel, place, arrays, shapes, scratch):
    return pl.pallas_call(
        kernel,
        in_specs=[SMEM] + [VMEM] * len(arrays),
        out_specs=[VMEM] * len(shapes),
        out_shape=[jax.ShapeDtypeStruct(shape, F32) for shape in shapes],
        scratch_shapes=[pltpu.VMEM(shape, F32) for shape in scratch],
        compiler_params=pltpu.CompilerParams(vmem_limit_bytes=4 << 20),
    )(place, *arrays)


def vocab_grad_kernel(lines, weights, out):
    out[...] = lax.dot_general(
        lines[...], weights[...], (((0,), (0,)), ((), ())), preferred_element_type=F32
    ).astype(out.dtype)


def vocab_grad_of(lines, weights):
    (rows, width), cols, step = lines.shape, weights.shape[1], 512
    return pl.pallas_call(
        vocab_grad_kernel,
        grid=(width // step,),
        in_specs=[
            pl.BlockSpec((rows, step), lambda i: (0, i)),
            pl.BlockSpec((rows, cols), lambda i: (0, 0)),
        ],
        out_specs=pl.BlockSpec((step, cols), lambda i: (i, 0)),
        out_shape=jax.ShapeDtypeStruct((width, cols), BF16),
        compiler_params=pltpu.CompilerParams(vmem_limit_bytes=16 << 20),
        cost_estimate=pl.CostEstimate(
            flops=2 * rows * width * cols, transcendentals=0, bytes_accessed=12 << 20
        ),
        name="vocab_grad",
    )(lines, weights)


def weight_of(score, goal, log_total):
    factor = 1.0 + 2.0 * PENALTY * log_total
    columns = lax.broadcasted_iota(jnp.int32, score.shape, 1)
    hit = (columns == goal).astype(F32)
    return (jnp.exp(score - log_total) * factor - hit).astype(BF16)


def per_device(stream, norm_gain, vocab_matrix, column_bias, targets):
    zs, xs = lax.axis_size("z"), 4
    mid = zs // 2
    my_rows, width = stream.shape
    cols = vocab_matrix.shape[1]
    xp, xm, core = lax.axis_index("xp"), lax.axis_index("xm"), lax.axis_index("c")
    x = 2 * xp + xm
    order = stage_rows(zs)

    normin = stream.astype(F32)
    inverse = lax.rsqrt(jnp.mean(normin * normin, axis=1, keepdims=True) + EPSILON)
    normed = (normin * inverse * norm_gain).astype(BF16)

    beside = shift(normed, "xm", 1)
    across = [(2 * i, 2 * i) for i in range(xs)] + [(2 * i + 1, 2 * (3 - i) + 1) for i in range(xs)]
    vocab = lax.ppermute(vocab_matrix, (*X, "c"), across)
    bias = lax.ppermute(column_bias, (*X, "c"), across)[None]
    shard = lax.axis_index("z") * xs + jnp.where(core == 0, x, 3 - x)

    my_goals = lax.dynamic_slice_in_dim(targets.reshape(zs, xs, my_rows), 2 * xp, 2, 1)
    far_goals = shift(my_goals, "c", 1)
    goals = jnp.stack([my_goals, far_goals]) - shard * cols
    goals = mirrored(mirrored(goals, "z", 1), "xm", 2).reshape(2, zs, 2 * my_rows)
    goals = jnp.concatenate([goals[line] for line in order]).reshape(-1, 1)

    own, far, stats = {}, {}, []

    def arrive(chain, distance, chunk):
        own[chain, distance] = chunk
        far[chain, distance] = shift(chunk, "c", 1)

    def distances(step):
        return sorted({step, (zs - step) % zs})

    def score_now(step, held):
        chunks = [held_by[chain, k] for held_by in (own, far) for k in distances(step) for chain in range(2)]
        first = order.index((0, distances(step)[0])) * 2 * my_rows
        lines, scores, stat = score_stage(chunks, vocab, bias, goals, first, held)
        stats.append(stat)
        return lines, scores

    heads = [(normed, normed), (beside, beside)]
    arrive(0, 0, normed)
    arrive(1, 0, beside)
    held = ()
    for step in range(1, mid):
        for chain in range(2):
            up, down = heads[chain]
            up, down = shift(up, "z", 1), shift(down, "z", -1)
            if chain == 1 and step >= 2:
                held = score_now(step - 2, held)
                up, down, *held = lax.optimization_barrier((up, down, *held))
            else:
                up, down = lax.optimization_barrier((up, down))
            heads[chain] = up, down
            arrive(chain, step, up)
            arrive(chain, zs - step, down)
    low, high = shift(heads[0][0], "z", 1), shift(heads[1][1], "z", -1)
    held = score_now(mid - 2, held)
    low, high, *held = lax.optimization_barrier((low, high, *held))
    arrive(0, mid, low)
    arrive(1, mid, high)
    held = score_now(mid - 1, held)
    lines, scores = score_now(mid, held)

    place = jnp.stack([core, lax.axis_index("z"), xm]).astype(jnp.int32)
    by_distance, by_owner = (2, zs, 2 * my_rows), (2 * zs, 2 * my_rows)
    (sent,) = small_call(
        functools.partial(pack_kernel, len(stats)),
        place,
        stats,
        [(4 * zs, 2 * zs + 1, 2 * my_rows)],
        [by_distance, by_distance, by_owner],
    )
    got = lax.all_to_all(sent, GROUP, 0, 0, tiled=True)
    totals, losses = small_call(
        unpack_kernel, place, [got], [by_owner, (1, 2 * my_rows)], [by_owner]
    )
    losses = losses[0, :my_rows]
    weights = weight_of(scores, goals, totals.reshape(-1, 1))

    def rows_of(row, count, weights):
        return lax.dot_general(
            weights[row : row + count],
            vocab,
            (((1,), (1,)), ((), ())),
            preferred_element_type=F32,
        )

    def cross(step, weights):
        lots = distances(step)
        row = order.index((1, lots[0])) * 2 * my_rows
        part = rows_of(row, len(lots) * 2 * my_rows, weights)
        return shift(part, "c", 1)

    def part_of(crossed, distance, weights, low=0, high=2 * my_rows):
        row = order.index((0, distance)) * 2 * my_rows
        return rows_of(row + low, high - low, weights) + crossed[low:high]

    crossed = cross(mid, weights)
    up = part_of(crossed, mid, weights, high=my_rows).astype(BF16)
    down = part_of(crossed, mid, weights, low=my_rows).astype(BF16)
    up, down, weights = lax.optimization_barrier((up, down, weights))
    up, down = shift(up, "z", 1), shift(down, "z", -1)
    local_grad = vocab_grad_of(lines, weights)
    up, down, local_grad = lax.optimization_barrier((up, down, local_grad))
    up = jnp.pad(up.astype(F32), ((0, my_rows), (0, 0)))
    down = jnp.pad(down.astype(F32), ((my_rows, 0), (0, 0)))
    for step in range(1, mid):
        crossed = cross(mid - step, weights)
        behind, ahead = crossed[: 2 * my_rows], crossed[2 * my_rows :]
        up = (part_of(ahead, mid + step, weights) + up).astype(BF16)
        down = (part_of(behind, mid - step, weights) + down).astype(BF16)
        up, down, weights = lax.optimization_barrier((up, down, weights))
        up, down = shift(up, "z", 1), shift(down, "z", -1)
        up, down = lax.optimization_barrier((up, down))
        up, down = up.astype(F32), down.astype(F32)
    pair_sum = part_of(cross(0, weights), 0, weights) + up + down
    rows_grad = pair_sum[:my_rows] + shift(pair_sum[my_rows:].astype(BF16), "xm", 1).astype(F32)

    ys = lax.axis_size("y")
    parts = local_grad.reshape(ys, width // ys, cols)
    arrived = lax.all_to_all(parts, "y", 0, 0, tiled=True)
    blocks = jnp.sum(arrived.astype(F32), axis=0).reshape(2, -1, cols)
    home = [(2 * i, 2 * i + 1) for i in range(xs)] + [(2 * i + 1, 2 * (3 - i)) for i in range(xs)]
    first = lax.dynamic_slice_in_dim(blocks, 1 - core, 1, 0)[0]
    second = lax.dynamic_slice_in_dim(blocks, core, 1, 0)[0]
    vocab_grad = lax.ppermute(first, (*X, "c"), home) + lax.ppermute(second, (*X, "c"), across)

    scaled = rows_grad * norm_gain
    projected = jnp.mean(scaled * normin, axis=1, keepdims=True)
    normin_grad = inverse * (scaled - normin * inverse * inverse * projected)
    return (losses, normin_grad, vocab_grad)


def solution(mesh):
    torus = Mesh(mesh.devices.reshape(8, 2, 2, 4, 2), ("z", "xp", "xm", "y", "c"))
    everyone = DP + VP
    in_specs = (P(everyone, None), P(), P(None, VP), P(VP), P(DP))
    out_specs = (P(everyone), P(everyone, None), P(DP, VP))

    return jax.shard_map(
        per_device, mesh=torus, in_specs=in_specs, out_specs=out_specs, check_vma=False
    )
```

```python
import functools

import jax
import jax.numpy as jnp
from jax import lax
from jax.experimental import pallas as pl
from jax.experimental.pallas import tpu as pltpu
from jax.sharding import Mesh
from jax.sharding import PartitionSpec as P

PENALTY = 0.001
EPSILON = 1e-06
BF16 = jnp.bfloat16
F32 = jnp.float32
X = ("xp", "xm")
VP = ("z", *X)
DP = ("y", "c")
GROUP = ("c", "z", "xm")
LANES = 128
ANY = pl.BlockSpec(memory_space=pl.ANY)
HBM = pl.BlockSpec(memory_space=pltpu.HBM)
VMEM = pl.BlockSpec(memory_space=pltpu.VMEM)
SMEM = pl.BlockSpec(memory_space=pltpu.SMEM)


def shift(value, axis, step):
    size = lax.axis_size(axis)
    return lax.ppermute(value, axis, [(i, (i + step) % size) for i in range(size)])


def mirrored(value, axis, dim):
    size = lax.axis_size(axis)
    flipped = jnp.flip(value, dim)
    start = size - 1 - lax.axis_index(axis)
    return lax.dynamic_slice_in_dim(jnp.concatenate([flipped, flipped], dim), start, size, dim)


def turned(row, place):
    return jnp.where(place[2] == 1, pltpu.roll(row, row.shape[1] // 2, 1), row)


def score_kernel(n, first, *refs):
    chunks, (vocab, bias, goals) = refs[:n], refs[n : n + 3]
    lines, scores, stats, x_buf, s_buf, sems = refs[-6:]
    rows = x_buf.shape[0]
    copies, row = [], 0
    for i, chunk in enumerate(chunks):
        place = x_buf.at[pl.ds(row, chunk.shape[0])]
        copies.append(pltpu.make_async_copy(chunk, place, sems.at[i]))
        row += chunk.shape[0]
    for copy in copies:
        copy.start()
    for copy in copies:
        copy.wait()
    out_x = pltpu.make_async_copy(x_buf, lines.at[pl.ds(first, rows)], sems.at[n])
    out_x.start()
    s_buf[...] = jnp.dot(x_buf[...], vocab[...], preferred_element_type=F32) + bias[...]
    out_s = pltpu.make_async_copy(s_buf, scores.at[pl.ds(first, rows)], sems.at[n + 1])
    out_s.start()
    diagonal = lax.broadcasted_iota(jnp.int32, (LANES, LANES), 0) == lax.broadcasted_iota(
        jnp.int32, (LANES, LANES), 1
    )

    def across(column):
        return jnp.sum(jnp.where(diagonal, column, 0.0), axis=0, keepdims=True)

    for g in range(rows // LANES):
        at = pl.ds(g * LANES, LANES)
        score = s_buf[at, :]
        top = jnp.max(score, axis=1, keepdims=True)
        total = jnp.sum(jnp.exp(score - top), axis=1, keepdims=True)
        hit = lax.broadcasted_iota(jnp.int32, score.shape, 1) == goals[at, :]
        pick = jnp.sum(jnp.where(hit, score, 0.0), axis=1, keepdims=True)
        stats[0, g : g + 1, :] = across(top + jnp.log(total))
        stats[1, g : g + 1, :] = across(pick)
    out_x.wait()
    out_s.wait()


def score_stage(chunks, vocab, bias, goals, first, held):
    rows = sum(chunk.shape[0] for chunk in chunks)
    n, (width, cols), every = len(chunks), vocab.shape, goals.shape[0]
    goal_block = pl.BlockSpec((rows, 1), lambda: (0, 0))
    return pl.pallas_call(
        functools.partial(score_kernel, n, first),
        in_specs=[ANY] * n + [VMEM, VMEM, goal_block] + [HBM, ANY][: len(held)],
        out_specs=[HBM, ANY, VMEM],
        out_shape=[
            pltpu.HBM((every, width), BF16),
            pltpu.HBM((every, cols), F32),
            jax.ShapeDtypeStruct((2, rows // LANES, LANES), F32),
        ],
        scratch_shapes=[
            pltpu.VMEM((rows, width), BF16),
            pltpu.VMEM((rows, cols), F32),
            pltpu.SemaphoreType.DMA((n + 2,)),
        ],
        input_output_aliases={n + 3 + i: i for i in range(len(held))},
        compiler_params=pltpu.CompilerParams(vmem_limit_bytes=14 << 20),
        cost_estimate=pl.CostEstimate(
            flops=2 * rows * width * cols, transcendentals=rows * cols, bytes_accessed=8 << 20
        ),
        name="score",
    )(*chunks, vocab, bias, lax.slice_in_dim(goals, first, first + rows, axis=0), *held)


def stage_rows(zs):
    found = []
    for step in range(zs // 2 + 1):
        distances = sorted({step, (zs - step) % zs})
        found += [(side, k) for side in range(2) for k in distances]
    return found


def pack_kernel(n, place, *refs):
    stats, (sent, spans, hits, joined) = refs[:n], refs[n:]
    zs = spans.shape[1]
    order, group = stage_rows(zs), 0
    for stat in stats:
        for g in range(stat.shape[1]):
            side, k = order[group]
            spans[side, k : k + 1, :] = stat[0, g : g + 1, :]
            hits[side, k : k + 1, :] = stat[1, g : g + 1, :]
            group += 1
    for side in range(2):
        for z in range(zs):
            line = (place[0] ^ side, pl.ds((place[1] + zs - z) % zs, 1))
            span, hit = turned(spans[line], place), turned(hits[line], place)
            at = side * zs + z
            joined[at : at + 1, :] = span
            sent[2 * at, 2 * zs :, :] = hit
            sent[2 * at + 1, 2 * zs :, :] = pltpu.roll(hit, hit.shape[1] // 2, 1)
    everyone = joined[...]
    for device in range(sent.shape[0]):
        sent[device, : 2 * zs, :] = everyone


def unpack_kernel(place, got, totals, losses, held):
    zs = held.shape[0] // 2
    spans = got[:, : 2 * zs, :]
    top = jnp.max(spans, axis=0)
    held[...] = top + jnp.log(jnp.sum(jnp.exp(spans - top[None]), axis=0))
    for group, (side, k) in enumerate(stage_rows(zs)):
        row = (place[0] ^ side) * zs + (place[1] + zs - k) % zs
        totals[group : group + 1, :] = turned(held[pl.ds(row, 1), :], place)
    own = turned(held[pl.ds(place[0] * zs + place[1], 1), :], place)
    picked = jnp.sum(got[:, 2 * zs :, :], axis=0)
    losses[...] = own - picked + PENALTY * own * own


def small_call(kernel, place, arrays, shapes, scratch):
    return pl.pallas_call(
        kernel,
        in_specs=[SMEM] + [VMEM] * len(arrays),
        out_specs=[VMEM] * len(shapes),
        out_shape=[jax.ShapeDtypeStruct(shape, F32) for shape in shapes],
        scratch_shapes=[pltpu.VMEM(shape, F32) for shape in scratch],
        compiler_params=pltpu.CompilerParams(vmem_limit_bytes=4 << 20),
    )(place, *arrays)


def vocab_grad_kernel(lines, weights, out):
    out[...] = lax.dot_general(
        lines[...], weights[...], (((0,), (0,)), ((), ())), preferred_element_type=F32
    ).astype(out.dtype)


def vocab_grad_of(lines, weights):
    (rows, width), cols, step = lines.shape, weights.shape[1], 512
    return pl.pallas_call(
        vocab_grad_kernel,
        grid=(width // step,),
        in_specs=[
            pl.BlockSpec((rows, step), lambda i: (0, i)),
            pl.BlockSpec((rows, cols), lambda i: (0, 0)),
        ],
        out_specs=pl.BlockSpec((step, cols), lambda i: (i, 0)),
        out_shape=jax.ShapeDtypeStruct((width, cols), BF16),
        compiler_params=pltpu.CompilerParams(vmem_limit_bytes=16 << 20),
        cost_estimate=pl.CostEstimate(
            flops=2 * rows * width * cols, transcendentals=0, bytes_accessed=12 << 20
        ),
        name="vocab_grad",
    )(lines, weights)


def weight_of(score, goal, log_total):
    factor = 1.0 + 2.0 * PENALTY * log_total
    columns = lax.broadcasted_iota(jnp.int32, score.shape, 1)
    hit = (columns == goal).astype(F32)
    return (jnp.exp(score - log_total) * factor - hit).astype(BF16)


def per_device(stream, norm_gain, vocab_matrix, column_bias, targets):
    zs, xs = lax.axis_size("z"), 4
    mid = zs // 2
    my_rows, width = stream.shape
    cols = vocab_matrix.shape[1]
    xp, xm, core = lax.axis_index("xp"), lax.axis_index("xm"), lax.axis_index("c")
    x = 2 * xp + xm
    order = stage_rows(zs)

    normin = stream.astype(F32)
    inverse = lax.rsqrt(jnp.mean(normin * normin, axis=1, keepdims=True) + EPSILON)
    normed = (normin * inverse * norm_gain).astype(BF16)

    beside = shift(normed, "xm", 1)
    across = [(2 * i, 2 * i) for i in range(xs)] + [(2 * i + 1, 2 * (3 - i) + 1) for i in range(xs)]
    vocab = lax.ppermute(vocab_matrix, (*X, "c"), across)
    bias = lax.ppermute(column_bias, (*X, "c"), across)[None]
    shard = lax.axis_index("z") * xs + jnp.where(core == 0, x, 3 - x)

    my_goals = lax.dynamic_slice_in_dim(targets.reshape(zs, xs, my_rows), 2 * xp, 2, 1)
    far_goals = shift(my_goals, "c", 1)
    goals = jnp.stack([my_goals, far_goals]) - shard * cols
    goals = mirrored(mirrored(goals, "z", 1), "xm", 2).reshape(2, zs, 2 * my_rows)
    goals = jnp.concatenate([goals[line] for line in order]).reshape(-1, 1)

    own, far, stats = {}, {}, []

    def arrive(chain, distance, chunk):
        own[chain, distance] = chunk
        far[chain, distance] = shift(chunk, "c", 1)

    def distances(step):
        return sorted({step, (zs - step) % zs})

    def score_now(step, held):
        chunks = [held_by[chain, k] for held_by in (own, far) for k in distances(step) for chain in range(2)]
        first = order.index((0, distances(step)[0])) * 2 * my_rows
        lines, scores, stat = score_stage(chunks, vocab, bias, goals, first, held)
        stats.append(stat)
        return lines, scores

    heads = [(normed, normed), (beside, beside)]
    arrive(0, 0, normed)
    arrive(1, 0, beside)
    held = ()
    for step in range(1, mid):
        for chain in range(2):
            up, down = heads[chain]
            up, down = shift(up, "z", 1), shift(down, "z", -1)
            if chain == 1 and step >= 2:
                held = score_now(step - 2, held)
                up, down, *held = lax.optimization_barrier((up, down, *held))
            else:
                up, down = lax.optimization_barrier((up, down))
            heads[chain] = up, down
            arrive(chain, step, up)
            arrive(chain, zs - step, down)
    low, high = shift(heads[0][0], "z", 1), shift(heads[1][1], "z", -1)
    held = score_now(mid - 2, held)
    low, high, *held = lax.optimization_barrier((low, high, *held))
    arrive(0, mid, low)
    arrive(1, mid, high)
    held = score_now(mid - 1, held)
    lines, scores = score_now(mid, held)

    place = jnp.stack([core, lax.axis_index("z"), xm]).astype(jnp.int32)
    by_distance, by_owner = (2, zs, 2 * my_rows), (2 * zs, 2 * my_rows)
    (sent,) = small_call(
        functools.partial(pack_kernel, len(stats)),
        place,
        stats,
        [(4 * zs, 2 * zs + 1, 2 * my_rows)],
        [by_distance, by_distance, by_owner],
    )
    got = lax.all_to_all(sent, GROUP, 0, 0, tiled=True)
    totals, losses = small_call(
        unpack_kernel, place, [got], [by_owner, (1, 2 * my_rows)], [by_owner]
    )
    losses = losses[0, :my_rows]
    block = 2 * my_rows

    def rows_of(weights, row, count):
        return lax.dot_general(
            weights[row : row + count],
            vocab,
            (((1,), (1,)), ((), ())),
            preferred_element_type=F32,
        )

    def cross(weights, step, start=0):
        lots = distances(step)
        row = order.index((1, lots[0])) * block - start
        part = rows_of(weights, row, len(lots) * block)
        return shift(part, "c", 1)

    def part_of(weights, crossed, distance, low=0, high=block, start=0):
        row = order.index((0, distance)) * block - start
        return rows_of(weights, row + low, high - low) + crossed[low:high]

    start = order.index((0, mid)) * block
    last = weight_of(scores[start:], goals[start:], totals[start // block :].reshape(-1, 1))
    crossed = cross(last, mid, start)
    up = part_of(last, crossed, mid, high=my_rows, start=start).astype(BF16)
    down = part_of(last, crossed, mid, low=my_rows, start=start).astype(BF16)
    up, down, totals = lax.optimization_barrier((up, down, totals))
    up, down = shift(up, "z", 1), shift(down, "z", -1)
    weights = weight_of(scores, goals, totals.reshape(-1, 1))
    up, down = lax.optimization_barrier((up, down))
    up = jnp.pad(up.astype(F32), ((0, my_rows), (0, 0)))
    down = jnp.pad(down.astype(F32), ((my_rows, 0), (0, 0)))
    crossed = cross(weights, mid - 1)
    ahead = part_of(weights, crossed[block:], mid + 1)
    behind = part_of(weights, crossed[:block], mid - 1)
    for step in range(1, mid):
        up, down = (ahead + up).astype(BF16), (behind + down).astype(BF16)
        up, down, weights = lax.optimization_barrier((up, down, weights))
        up, down = shift(up, "z", 1), shift(down, "z", -1)
        if step == 1:
            local_grad = vocab_grad_of(lines, weights)
        crossed = cross(weights, mid - step - 1)
        behind = part_of(weights, crossed[:block], mid - step - 1)
        if step + 1 < mid:
            ahead = part_of(weights, crossed[block:], mid + step + 1)
        ahead, behind = lax.optimization_barrier((ahead, behind))
        up, down = lax.optimization_barrier((up, down))
        up, down = up.astype(F32), down.astype(F32)
    pair_sum = behind + up + down
    rows_grad = pair_sum[:my_rows] + shift(pair_sum[my_rows:].astype(BF16), "xm", 1).astype(F32)

    ys = lax.axis_size("y")
    parts = local_grad.reshape(ys, width // ys, cols)
    arrived = lax.all_to_all(parts, "y", 0, 0, tiled=True)
    blocks = jnp.sum(arrived.astype(F32), axis=0).reshape(2, -1, cols)
    home = [(2 * i, 2 * i + 1) for i in range(xs)] + [(2 * i + 1, 2 * (3 - i)) for i in range(xs)]
    first = lax.dynamic_slice_in_dim(blocks, 1 - core, 1, 0)[0]
    second = lax.dynamic_slice_in_dim(blocks, core, 1, 0)[0]
    vocab_grad = lax.ppermute(first, (*X, "c"), home) + lax.ppermute(second, (*X, "c"), across)

    scaled = rows_grad * norm_gain
    projected = jnp.mean(scaled * normin, axis=1, keepdims=True)
    normin_grad = inverse * (scaled - normin * inverse * inverse * projected)
    return (losses, normin_grad, vocab_grad)


def solution(mesh):
    torus = Mesh(mesh.devices.reshape(8, 2, 2, 4, 2), ("z", "xp", "xm", "y", "c"))
    everyone = DP + VP
    in_specs = (P(everyone, None), P(), P(None, VP), P(VP), P(DP))
    out_specs = (P(everyone), P(everyone, None), P(DP, VP))

    return jax.shard_map(
        per_device, mesh=torus, in_specs=in_specs, out_specs=out_specs, check_vma=False
    )
```

```python
import functools

import jax
import jax.numpy as jnp
from jax import lax
from jax.experimental import pallas as pl
from jax.experimental.pallas import tpu as pltpu
from jax.sharding import Mesh
from jax.sharding import PartitionSpec as P

PENALTY = 0.001
EPSILON = 1e-06
BF16 = jnp.bfloat16
F32 = jnp.float32
X = ("xp", "xm")
VP = ("z", *X)
DP = ("y", "c")
GROUP = ("c", "z", "xm")
LANES = 128
ANY = pl.BlockSpec(memory_space=pl.ANY)
HBM = pl.BlockSpec(memory_space=pltpu.HBM)
VMEM = pl.BlockSpec(memory_space=pltpu.VMEM)
SMEM = pl.BlockSpec(memory_space=pltpu.SMEM)


def shift(value, axis, step):
    size = lax.axis_size(axis)
    return lax.ppermute(value, axis, [(i, (i + step) % size) for i in range(size)])


def mirrored(value, axis, dim):
    size = lax.axis_size(axis)
    flipped = jnp.flip(value, dim)
    start = size - 1 - lax.axis_index(axis)
    return lax.dynamic_slice_in_dim(jnp.concatenate([flipped, flipped], dim), start, size, dim)


def turned(row, place):
    return jnp.where(place[2] == 1, pltpu.roll(row, row.shape[1] // 2, 1), row)


def score_kernel(n, first, *refs):
    chunks, (vocab, bias, goals) = refs[:n], refs[n : n + 3]
    lines, scores, stats, x_buf, s_buf, sems = refs[-6:]
    rows = x_buf.shape[0]
    copies, row = [], 0
    for i, chunk in enumerate(chunks):
        place = x_buf.at[pl.ds(row, chunk.shape[0])]
        copies.append(pltpu.make_async_copy(chunk, place, sems.at[i]))
        row += chunk.shape[0]
    for copy in copies:
        copy.start()
    for copy in copies:
        copy.wait()
    out_x = pltpu.make_async_copy(x_buf, lines.at[pl.ds(first, rows)], sems.at[n])
    out_x.start()
    s_buf[...] = jnp.dot(x_buf[...], vocab[...], preferred_element_type=F32) + bias[...]
    out_s = pltpu.make_async_copy(s_buf, scores.at[pl.ds(first, rows)], sems.at[n + 1])
    out_s.start()
    diagonal = lax.broadcasted_iota(jnp.int32, (LANES, LANES), 0) == lax.broadcasted_iota(
        jnp.int32, (LANES, LANES), 1
    )

    def across(column):
        return jnp.sum(jnp.where(diagonal, column, 0.0), axis=0, keepdims=True)

    def group(g, carry):
        at = pl.ds(pl.multiple_of(g * LANES, LANES), LANES)
        score = s_buf[at, :]
        top = jnp.max(score, axis=1, keepdims=True)
        total = jnp.sum(jnp.exp(score - top), axis=1, keepdims=True)
        hit = lax.broadcasted_iota(jnp.int32, score.shape, 1) == goals[at, :]
        pick = jnp.sum(jnp.where(hit, score, 0.0), axis=1, keepdims=True)
        stats[0, pl.ds(g, 1), :] = across(top + jnp.log(total))
        stats[1, pl.ds(g, 1), :] = across(pick)
        return carry

    lax.fori_loop(0, rows // LANES, group, 0)
    out_x.wait()
    out_s.wait()


def score_stage(chunks, vocab, bias, goals, first, held):
    rows = sum(chunk.shape[0] for chunk in chunks)
    n, (width, cols), every = len(chunks), vocab.shape, goals.shape[0]
    goal_block = pl.BlockSpec((rows, 1), lambda: (0, 0))
    return pl.pallas_call(
        functools.partial(score_kernel, n, first),
        in_specs=[ANY] * n + [VMEM, VMEM, goal_block] + [HBM] * len(held),
        out_specs=[HBM, HBM, VMEM],
        out_shape=[
            pltpu.HBM((every, width), BF16),
            pltpu.HBM((every, cols), F32),
            jax.ShapeDtypeStruct((2, rows // LANES, LANES), F32),
        ],
        scratch_shapes=[
            pltpu.VMEM((rows, width), BF16),
            pltpu.VMEM((rows, cols), F32),
            pltpu.SemaphoreType.DMA((n + 2,)),
        ],
        input_output_aliases={n + 3 + i: i for i in range(len(held))},
        compiler_params=pltpu.CompilerParams(vmem_limit_bytes=14 << 20),
        cost_estimate=pl.CostEstimate(
            flops=2 * rows * width * cols, transcendentals=rows * cols, bytes_accessed=8 << 20
        ),
        name="score",
    )(*chunks, vocab, bias, lax.slice_in_dim(goals, first, first + rows, axis=0), *held)


def stage_rows(zs):
    found = []
    for step in range(zs // 2 + 1):
        distances = sorted({step, (zs - step) % zs})
        found += [(side, k) for side in range(2) for k in distances]
    return found


def pack_kernel(n, place, *refs):
    stats, (sent, spans, hits, joined) = refs[:n], refs[n:]
    zs = spans.shape[1]
    order, group = stage_rows(zs), 0
    for stat in stats:
        for g in range(stat.shape[1]):
            side, k = order[group]
            spans[side, k : k + 1, :] = stat[0, g : g + 1, :]
            hits[side, k : k + 1, :] = stat[1, g : g + 1, :]
            group += 1
    for side in range(2):
        for z in range(zs):
            line = (place[0] ^ side, pl.ds((place[1] + zs - z) % zs, 1))
            span, hit = turned(spans[line], place), turned(hits[line], place)
            at = side * zs + z
            joined[at : at + 1, :] = span
            sent[2 * at, 2 * zs :, :] = hit
            sent[2 * at + 1, 2 * zs :, :] = pltpu.roll(hit, hit.shape[1] // 2, 1)
    everyone = joined[...]
    for device in range(sent.shape[0]):
        sent[device, : 2 * zs, :] = everyone


def unpack_kernel(place, got, totals, losses, held):
    zs = held.shape[0] // 2
    spans = got[:, : 2 * zs, :]
    top = jnp.max(spans, axis=0)
    held[...] = top + jnp.log(jnp.sum(jnp.exp(spans - top[None]), axis=0))
    for group, (side, k) in enumerate(stage_rows(zs)):
        row = (place[0] ^ side) * zs + (place[1] + zs - k) % zs
        totals[group : group + 1, :] = turned(held[pl.ds(row, 1), :], place)
    own = turned(held[pl.ds(place[0] * zs + place[1], 1), :], place)
    picked = jnp.sum(got[:, 2 * zs :, :], axis=0)
    losses[...] = own - picked + PENALTY * own * own


def small_call(kernel, place, arrays, shapes, scratch):
    return pl.pallas_call(
        kernel,
        in_specs=[SMEM] + [VMEM] * len(arrays),
        out_specs=[VMEM] * len(shapes),
        out_shape=[jax.ShapeDtypeStruct(shape, F32) for shape in shapes],
        scratch_shapes=[pltpu.VMEM(shape, F32) for shape in scratch],
        compiler_params=pltpu.CompilerParams(vmem_limit_bytes=4 << 20),
    )(place, *arrays)


def vocab_grad_kernel(lines, weights, out):
    out[...] = lax.dot_general(
        lines[...], weights[...], (((0,), (0,)), ((), ())), preferred_element_type=F32
    ).astype(out.dtype)


def vocab_grad_of(lines, weights):
    (rows, width), cols, step = lines.shape, weights.shape[1], 512
    return pl.pallas_call(
        vocab_grad_kernel,
        grid=(width // step,),
        in_specs=[
            pl.BlockSpec((rows, step), lambda i: (0, i)),
            pl.BlockSpec((rows, cols), lambda i: (0, 0)),
        ],
        out_specs=pl.BlockSpec((step, cols), lambda i: (i, 0)),
        out_shape=pltpu.HBM((width, cols), BF16),
        compiler_params=pltpu.CompilerParams(vmem_limit_bytes=16 << 20),
        cost_estimate=pl.CostEstimate(
            flops=2 * rows * width * cols, transcendentals=0, bytes_accessed=12 << 20
        ),
        name="vocab_grad",
    )(lines, weights)


def weight_of(score, goal, log_total):
    factor = 1.0 + 2.0 * PENALTY * log_total
    columns = lax.broadcasted_iota(jnp.int32, score.shape, 1)
    hit = (columns == goal).astype(F32)
    return (jnp.exp(score - log_total) * factor - hit).astype(BF16)


def per_device(stream, norm_gain, vocab_matrix, column_bias, targets):
    zs, xs = lax.axis_size("z"), 4
    mid = zs // 2
    my_rows, width = stream.shape
    cols = vocab_matrix.shape[1]
    xp, xm, core = lax.axis_index("xp"), lax.axis_index("xm"), lax.axis_index("c")
    x = 2 * xp + xm
    order = stage_rows(zs)

    normin = stream.astype(F32)
    inverse = lax.rsqrt(jnp.mean(normin * normin, axis=1, keepdims=True) + EPSILON)
    normed = (normin * inverse * norm_gain).astype(BF16)

    beside = shift(normed, "xm", 1)
    across = [(2 * i, 2 * i) for i in range(xs)] + [(2 * i + 1, 2 * (3 - i) + 1) for i in range(xs)]
    vocab = lax.ppermute(vocab_matrix, (*X, "c"), across)
    bias = lax.ppermute(column_bias, (*X, "c"), across)[None]
    shard = lax.axis_index("z") * xs + jnp.where(core == 0, x, 3 - x)

    my_goals = lax.dynamic_slice_in_dim(targets.reshape(zs, xs, my_rows), 2 * xp, 2, 1)
    far_goals = shift(my_goals, "c", 1)
    goals = jnp.stack([my_goals, far_goals]) - shard * cols
    goals = mirrored(mirrored(goals, "z", 1), "xm", 2).reshape(2, zs, 2 * my_rows)
    goals = jnp.concatenate([goals[line] for line in order]).reshape(-1, 1)

    own, far, stats = {}, {}, []

    def arrive(chain, distance, chunk):
        own[chain, distance] = chunk
        far[chain, distance] = shift(chunk, "c", 1)

    def distances(step):
        return sorted({step, (zs - step) % zs})

    def score_now(step, held):
        chunks = [held_by[chain, k] for held_by in (own, far) for k in distances(step) for chain in range(2)]
        first = order.index((0, distances(step)[0])) * 2 * my_rows
        lines, scores, stat = score_stage(chunks, vocab, bias, goals, first, held)
        stats.append(stat)
        return lines, scores

    heads = [(normed, normed), (beside, beside)]
    arrive(0, 0, normed)
    arrive(1, 0, beside)
    held = ()
    for step in range(1, mid):
        for chain in range(2):
            up, down = heads[chain]
            up, down = shift(up, "z", 1), shift(down, "z", -1)
            if chain == 1 and step >= 2:
                held = score_now(step - 2, held)
                up, down, *held = lax.optimization_barrier((up, down, *held))
            else:
                up, down = lax.optimization_barrier((up, down))
            heads[chain] = up, down
            arrive(chain, step, up)
            arrive(chain, zs - step, down)
    low, high = shift(heads[0][0], "z", 1), shift(heads[1][1], "z", -1)
    held = score_now(mid - 2, held)
    low, high, *held = lax.optimization_barrier((low, high, *held))
    arrive(0, mid, low)
    arrive(1, mid, high)
    held = score_now(mid - 1, held)
    lines, scores = score_now(mid, held)

    place = jnp.stack([core, lax.axis_index("z"), xm]).astype(jnp.int32)
    by_distance, by_owner = (2, zs, 2 * my_rows), (2 * zs, 2 * my_rows)
    (sent,) = small_call(
        functools.partial(pack_kernel, len(stats)),
        place,
        stats,
        [(4 * zs, 2 * zs + 1, 2 * my_rows)],
        [by_distance, by_distance, by_owner],
    )
    got = lax.all_to_all(sent, GROUP, 0, 0, tiled=True)
    totals, losses = small_call(
        unpack_kernel, place, [got], [by_owner, (1, 2 * my_rows)], [by_owner]
    )
    losses = losses[0, :my_rows]
    block = 2 * my_rows

    def rows_of(weights, row, count):
        return lax.dot_general(
            weights[row : row + count],
            vocab,
            (((1,), (1,)), ((), ())),
            preferred_element_type=F32,
        )

    def cross(weights, step, start=0):
        lots = distances(step)
        row = order.index((1, lots[0])) * block - start
        part = rows_of(weights, row, len(lots) * block)
        return shift(part, "c", 1)

    def part_of(weights, crossed, step, start=0):
        row = order.index((0, distances(step)[0])) * block - start
        return rows_of(weights, row, crossed.shape[0]) + crossed

    start = order.index((0, mid)) * block
    last = weight_of(scores[start:], goals[start:], totals[start // block :].reshape(-1, 1))
    crossed = cross(last, mid, start)
    both = part_of(last, crossed, mid, start).astype(BF16)
    up, down = both[:my_rows], both[my_rows:]
    up, down, totals = lax.optimization_barrier((up, down, totals))
    up, down = shift(up, "z", 1), shift(down, "z", -1)
    weights = weight_of(scores, goals, totals.reshape(-1, 1))
    up, down = lax.optimization_barrier((up, down))
    up = jnp.pad(up.astype(F32), ((0, my_rows), (0, 0)))
    down = jnp.pad(down.astype(F32), ((my_rows, 0), (0, 0)))
    crossed = cross(weights, mid - 1)
    base = part_of(weights, crossed, mid - 1)
    local_grad = vocab_grad_of(lines, weights)
    for step in range(1, mid - 1):
        up, down = (base[block:] + up).astype(BF16), (base[:block] + down).astype(BF16)
        up, down, weights = lax.optimization_barrier((up, down, weights))
        up, down = shift(up, "z", 1), shift(down, "z", -1)
        crossed = cross(weights, mid - step - 1)
        base = lax.optimization_barrier(part_of(weights, crossed, mid - step - 1))
        up, down = lax.optimization_barrier((up, down))
        up, down = up.astype(F32), down.astype(F32)
    ends = []
    for low in (my_rows, 0):
        rows, more = slice(low, low + my_rows), slice(block + low, block + low + my_rows)
        one, two = (base[more] + up[rows]).astype(BF16), (base[rows] + down[rows]).astype(BF16)
        one, two, weights = lax.optimization_barrier((one, two, weights))
        ends.append((shift(one, "z", 1), shift(two, "z", -1)))
    crossed = cross(weights, 0)
    base = lax.optimization_barrier(part_of(weights, crossed, 0))
    theirs = (base[my_rows:] + ends[0][0].astype(F32) + ends[0][1].astype(F32)).astype(BF16)
    theirs = shift(theirs, "xm", 1)
    mine = base[:my_rows] + ends[1][0].astype(F32) + ends[1][1].astype(F32)
    rows_grad = mine + theirs.astype(F32)

    ys = lax.axis_size("y")
    parts = local_grad.reshape(ys, width // ys, cols)
    arrived = lax.all_to_all(parts, "y", 0, 0, tiled=True)
    home = [(2 * i, 2 * i + 1) for i in range(xs)] + [(2 * i + 1, 2 * (3 - i)) for i in range(xs)]
    blocks = jnp.sum(arrived.astype(F32), axis=0).astype(BF16).reshape(2, -1, cols)
    first = lax.dynamic_slice_in_dim(blocks, 1 - core, 1, 0)[0]
    second = lax.dynamic_slice_in_dim(blocks, core, 1, 0)[0]
    first = lax.ppermute(first, (*X, "c"), home)
    second = lax.ppermute(second, (*X, "c"), across)
    vocab_grad = first.astype(F32) + second.astype(F32)

    scaled = rows_grad * norm_gain
    projected = jnp.mean(scaled * normin, axis=1, keepdims=True)
    normin_grad = inverse * (scaled - normin * inverse * inverse * projected)
    return (losses, normin_grad, vocab_grad)


def solution(mesh):
    torus = Mesh(mesh.devices.reshape(8, 2, 2, 4, 2), ("z", "xp", "xm", "y", "c"))
    everyone = DP + VP
    in_specs = (P(everyone, None), P(), P(None, VP), P(VP), P(DP))
    out_specs = (P(everyone), P(everyone, None), P(DP, VP))

    return jax.shard_map(
        per_device, mesh=torus, in_specs=in_specs, out_specs=out_specs, check_vma=False
    )
```

```python
import functools

import jax
import jax.numpy as jnp
from jax import lax
from jax.experimental import pallas as pl
from jax.experimental.pallas import tpu as pltpu
from jax.sharding import Mesh
from jax.sharding import PartitionSpec as P

PENALTY = 0.001
EPSILON = 1e-06
BF16 = jnp.bfloat16
F32 = jnp.float32
X = ("xp", "xm")
VP = ("z", *X)
DP = ("y", "c")
GROUP = ("c", "z", "xm")
LANES = 128
ANY = pl.BlockSpec(memory_space=pl.ANY)
HBM = pl.BlockSpec(memory_space=pltpu.HBM)
VMEM = pl.BlockSpec(memory_space=pltpu.VMEM)
SMEM = pl.BlockSpec(memory_space=pltpu.SMEM)


def shift(value, axis, step):
    size = lax.axis_size(axis)
    return lax.ppermute(value, axis, [(i, (i + step) % size) for i in range(size)])


def mirrored(value, axis, dim):
    size = lax.axis_size(axis)
    flipped = jnp.flip(value, dim)
    start = size - 1 - lax.axis_index(axis)
    return lax.dynamic_slice_in_dim(jnp.concatenate([flipped, flipped], dim), start, size, dim)


def turned(row, place):
    return jnp.where(place[2] == 1, pltpu.roll(row, row.shape[1] // 2, 1), row)


def score_kernel(n, first, *refs):
    chunks, (vocab, bias, goals) = refs[:n], refs[n : n + 3]
    lines, scores, stats, x_buf, s_buf, sems = refs[-6:]
    rows = x_buf.shape[0]
    copies, row = [], 0
    for i, chunk in enumerate(chunks):
        place = x_buf.at[pl.ds(row, chunk.shape[0])]
        copies.append(pltpu.make_async_copy(chunk, place, sems.at[i]))
        row += chunk.shape[0]
    for copy in copies:
        copy.start()
    for copy in copies:
        copy.wait()
    out_x = pltpu.make_async_copy(x_buf, lines.at[pl.ds(first, rows)], sems.at[n])
    out_x.start()
    s_buf[...] = jnp.dot(x_buf[...], vocab[...], preferred_element_type=F32) + bias[...]
    out_s = pltpu.make_async_copy(s_buf, scores.at[pl.ds(first, rows)], sems.at[n + 1])
    out_s.start()
    diagonal = lax.broadcasted_iota(jnp.int32, (LANES, LANES), 0) == lax.broadcasted_iota(
        jnp.int32, (LANES, LANES), 1
    )

    def across(column):
        return jnp.sum(jnp.where(diagonal, column, 0.0), axis=0, keepdims=True)

    def group(g, carry):
        at = pl.ds(pl.multiple_of(g * LANES, LANES), LANES)
        score = s_buf[at, :]
        top = jnp.max(score, axis=1, keepdims=True)
        total = jnp.sum(jnp.exp(score - top), axis=1, keepdims=True)
        hit = lax.broadcasted_iota(jnp.int32, score.shape, 1) == goals[at, :]
        pick = jnp.sum(jnp.where(hit, score, 0.0), axis=1, keepdims=True)
        stats[0, pl.ds(g, 1), :] = across(top + jnp.log(total))
        stats[1, pl.ds(g, 1), :] = across(pick)
        return carry

    lax.fori_loop(0, rows // LANES, group, 0)
    out_x.wait()
    out_s.wait()


def score_stage(chunks, vocab, bias, goals, first, held):
    rows = sum(chunk.shape[0] for chunk in chunks)
    n, (width, cols), every = len(chunks), vocab.shape, goals.shape[0]
    goal_block = pl.BlockSpec((rows, 1), lambda: (0, 0))
    return pl.pallas_call(
        functools.partial(score_kernel, n, first),
        in_specs=[ANY] * n + [VMEM, VMEM, goal_block] + [HBM] * len(held),
        out_specs=[HBM, HBM, VMEM],
        out_shape=[
            pltpu.HBM((every, width), BF16),
            pltpu.HBM((every, cols), F32),
            jax.ShapeDtypeStruct((2, rows // LANES, LANES), F32),
        ],
        scratch_shapes=[
            pltpu.VMEM((rows, width), BF16),
            pltpu.VMEM((rows, cols), F32),
            pltpu.SemaphoreType.DMA((n + 2,)),
        ],
        input_output_aliases={n + 3 + i: i for i in range(len(held))},
        compiler_params=pltpu.CompilerParams(vmem_limit_bytes=14 << 20),
        cost_estimate=pl.CostEstimate(
            flops=2 * rows * width * cols, transcendentals=rows * cols, bytes_accessed=8 << 20
        ),
        name="score",
    )(*chunks, vocab, bias, lax.slice_in_dim(goals, first, first + rows, axis=0), *held)


def stage_rows(zs):
    found = []
    for step in range(zs // 2 + 1):
        distances = sorted({step, (zs - step) % zs})
        found += [(side, k) for side in range(2) for k in distances]
    return found


def pack_kernel(n, place, *refs):
    stats, (sent, spans, hits, joined) = refs[:n], refs[n:]
    zs = spans.shape[1]
    order, group = stage_rows(zs), 0
    for stat in stats:
        for g in range(stat.shape[1]):
            side, k = order[group]
            spans[side, k : k + 1, :] = stat[0, g : g + 1, :]
            hits[side, k : k + 1, :] = stat[1, g : g + 1, :]
            group += 1
    for side in range(2):
        for z in range(zs):
            line = (place[0] ^ side, pl.ds((place[1] + zs - z) % zs, 1))
            span, hit = turned(spans[line], place), turned(hits[line], place)
            at = side * zs + z
            joined[at : at + 1, :] = span
            sent[2 * at, 2 * zs :, :] = hit
            sent[2 * at + 1, 2 * zs :, :] = pltpu.roll(hit, hit.shape[1] // 2, 1)
    everyone = joined[...]
    for device in range(sent.shape[0]):
        sent[device, : 2 * zs, :] = everyone


def unpack_kernel(place, got, totals, losses, held):
    zs = held.shape[0] // 2
    spans = got[:, : 2 * zs, :]
    top = jnp.max(spans, axis=0)
    held[...] = top + jnp.log(jnp.sum(jnp.exp(spans - top[None]), axis=0))
    for group, (side, k) in enumerate(stage_rows(zs)):
        row = (place[0] ^ side) * zs + (place[1] + zs - k) % zs
        totals[group : group + 1, :] = turned(held[pl.ds(row, 1), :], place)
    own = turned(held[pl.ds(place[0] * zs + place[1], 1), :], place)
    picked = jnp.sum(got[:, 2 * zs :, :], axis=0)
    losses[...] = own - picked + PENALTY * own * own


def small_call(kernel, place, arrays, shapes, scratch):
    return pl.pallas_call(
        kernel,
        in_specs=[SMEM] + [VMEM] * len(arrays),
        out_specs=[VMEM] * len(shapes),
        out_shape=[jax.ShapeDtypeStruct(shape, F32) for shape in shapes],
        scratch_shapes=[pltpu.VMEM(shape, F32) for shape in scratch],
        compiler_params=pltpu.CompilerParams(vmem_limit_bytes=4 << 20),
    )(place, *arrays)


def vocab_grad_kernel(lines, weights, out):
    out[...] = lax.dot_general(
        lines[...], weights[...], (((0,), (0,)), ((), ())), preferred_element_type=F32
    ).astype(out.dtype)


def vocab_grad_of(lines, weights):
    (rows, width), cols, step = lines.shape, weights.shape[1], 512
    return pl.pallas_call(
        vocab_grad_kernel,
        grid=(width // step,),
        in_specs=[
            pl.BlockSpec((rows, step), lambda i: (0, i)),
            pl.BlockSpec((rows, cols), lambda i: (0, 0)),
        ],
        out_specs=pl.BlockSpec((step, cols), lambda i: (i, 0)),
        out_shape=pltpu.HBM((width, cols), BF16),
        compiler_params=pltpu.CompilerParams(vmem_limit_bytes=16 << 20),
        cost_estimate=pl.CostEstimate(
            flops=2 * rows * width * cols, transcendentals=0, bytes_accessed=12 << 20
        ),
        name="vocab_grad",
    )(lines, weights)


def weight_of(score, goal, log_total):
    factor = 1.0 + 2.0 * PENALTY * log_total
    columns = lax.broadcasted_iota(jnp.int32, score.shape, 1)
    hit = (columns == goal).astype(F32)
    return (jnp.exp(score - log_total) * factor - hit).astype(BF16)


def per_device(stream, norm_gain, vocab_matrix, column_bias, targets):
    zs, xs = lax.axis_size("z"), 4
    mid = zs // 2
    my_rows, width = stream.shape
    cols = vocab_matrix.shape[1]
    xp, xm, core = lax.axis_index("xp"), lax.axis_index("xm"), lax.axis_index("c")
    x = 2 * xp + xm
    order = stage_rows(zs)

    normin = stream.astype(F32)
    inverse = lax.rsqrt(jnp.mean(normin * normin, axis=1, keepdims=True) + EPSILON)
    normed = (normin * inverse * norm_gain).astype(BF16)

    beside = shift(normed, "xm", 1)
    across = [(2 * i, 2 * i) for i in range(xs)] + [(2 * i + 1, 2 * (3 - i) + 1) for i in range(xs)]
    vocab = lax.ppermute(vocab_matrix, (*X, "c"), across)
    bias = lax.ppermute(column_bias, (*X, "c"), across)[None]
    shard = lax.axis_index("z") * xs + jnp.where(core == 0, x, 3 - x)

    my_goals = lax.dynamic_slice_in_dim(targets.reshape(zs, xs, my_rows), 2 * xp, 2, 1)
    far_goals = shift(my_goals, "c", 1)
    goals = jnp.stack([my_goals, far_goals]) - shard * cols
    goals = mirrored(mirrored(goals, "z", 1), "xm", 2).reshape(2, zs, 2 * my_rows)
    goals = jnp.concatenate([goals[line] for line in order]).reshape(-1, 1)

    own, far, stats = {}, {}, []

    def arrive(chain, distance, chunk):
        own[chain, distance] = chunk
        far[chain, distance] = shift(chunk, "c", 1)

    def distances(step):
        return sorted({step, (zs - step) % zs})

    def score_now(step, held):
        chunks = [held_by[chain, k] for held_by in (own, far) for k in distances(step) for chain in range(2)]
        first = order.index((0, distances(step)[0])) * 2 * my_rows
        lines, scores, stat = score_stage(chunks, vocab, bias, goals, first, held)
        stats.append(stat)
        return lines, scores

    heads = [(normed, normed), (beside, beside)]
    arrive(0, 0, normed)
    arrive(1, 0, beside)
    held = ()
    for step in range(1, mid):
        for chain in range(2):
            up, down = heads[chain]
            up, down = shift(up, "z", 1), shift(down, "z", -1)
            if chain == 1 and step >= 2:
                held = score_now(step - 2, held)
                up, down, *held = lax.optimization_barrier((up, down, *held))
            else:
                up, down = lax.optimization_barrier((up, down))
            heads[chain] = up, down
            arrive(chain, step, up)
            arrive(chain, zs - step, down)
    low, high = shift(heads[0][0], "z", 1), shift(heads[1][1], "z", -1)
    held = score_now(mid - 2, held)
    low, high, *held = lax.optimization_barrier((low, high, *held))
    arrive(0, mid, low)
    arrive(1, mid, high)
    held = score_now(mid - 1, held)
    lines, scores = score_now(mid, held)

    place = jnp.stack([core, lax.axis_index("z"), xm]).astype(jnp.int32)
    by_distance, by_owner = (2, zs, 2 * my_rows), (2 * zs, 2 * my_rows)
    (sent,) = small_call(
        functools.partial(pack_kernel, len(stats)),
        place,
        stats,
        [(4 * zs, 2 * zs + 1, 2 * my_rows)],
        [by_distance, by_distance, by_owner],
    )
    got = lax.all_to_all(sent, GROUP, 0, 0, tiled=True)
    totals, losses = small_call(
        unpack_kernel, place, [got], [by_owner, (1, 2 * my_rows)], [by_owner]
    )
    losses = losses[0, :my_rows]
    block = 2 * my_rows

    def rows_of(weights, row, count):
        return lax.dot_general(
            weights[row : row + count],
            vocab,
            (((1,), (1,)), ((), ())),
            preferred_element_type=F32,
        )

    def cross(weights, step, start=0):
        lots = distances(step)
        row = order.index((1, lots[0])) * block - start
        part = rows_of(weights, row, len(lots) * block)
        return shift(part, "c", 1)

    def part_of(weights, crossed, step, start=0):
        row = order.index((0, distances(step)[0])) * block - start
        return rows_of(weights, row, crossed.shape[0]) + crossed

    start = order.index((0, mid)) * block
    last = weight_of(scores[start:], goals[start:], totals[start // block :].reshape(-1, 1))
    crossed = cross(last, mid, start)
    both = part_of(last, crossed, mid, start).astype(BF16)
    up, down = both[:my_rows], both[my_rows:]
    up, down, totals = lax.optimization_barrier((up, down, totals))
    up, down = shift(up, "z", 1), shift(down, "z", -1)
    weights = weight_of(scores, goals, totals.reshape(-1, 1))
    up, down = lax.optimization_barrier((up, down))
    up = jnp.pad(up.astype(F32), ((0, my_rows), (0, 0)))
    down = jnp.pad(down.astype(F32), ((my_rows, 0), (0, 0)))
    crossed = cross(weights, mid - 1)
    base = part_of(weights, crossed, mid - 1)
    local_grad = vocab_grad_of(lines, weights)
    for step in range(1, mid - 1):
        up, down = (base[block:] + up).astype(BF16), (base[:block] + down).astype(BF16)
        up, down, weights = lax.optimization_barrier((up, down, weights))
        up, down = shift(up, "z", 1), shift(down, "z", -1)
        earlier = weights
        crossed = cross(weights, mid - step - 1)
        base = lax.optimization_barrier(part_of(weights, crossed, mid - step - 1))
        up, down = lax.optimization_barrier((up, down))
        up, down = up.astype(F32), down.astype(F32)
    crossed = cross(earlier, 0)
    final = lax.optimization_barrier(part_of(earlier, crossed, 0))
    ends = []
    for low in (my_rows, 0):
        rows, more = slice(low, low + my_rows), slice(block + low, block + low + my_rows)
        one, two = (base[more] + up[rows]).astype(BF16), (base[rows] + down[rows]).astype(BF16)
        one, two, weights = lax.optimization_barrier((one, two, weights))
        ends.append((shift(one, "z", 1), shift(two, "z", -1)))
    theirs = (final[my_rows:] + ends[0][0].astype(F32) + ends[0][1].astype(F32)).astype(BF16)
    theirs = shift(theirs, "xm", 1)
    mine = final[:my_rows] + ends[1][0].astype(F32) + ends[1][1].astype(F32)
    rows_grad = mine + theirs.astype(F32)

    ys = lax.axis_size("y")
    parts = local_grad.reshape(ys, width // ys, cols)
    arrived = lax.all_to_all(parts, "y", 0, 0, tiled=True)
    home = [(2 * i, 2 * i + 1) for i in range(xs)] + [(2 * i + 1, 2 * (3 - i)) for i in range(xs)]
    blocks = jnp.sum(arrived.astype(F32), axis=0).astype(BF16).reshape(2, -1, cols)
    first = lax.dynamic_slice_in_dim(blocks, 1 - core, 1, 0)[0]
    second = lax.dynamic_slice_in_dim(blocks, core, 1, 0)[0]
    first = lax.ppermute(first, (*X, "c"), home)
    second = lax.ppermute(second, (*X, "c"), across)
    vocab_grad = first.astype(F32) + second.astype(F32)

    scaled = rows_grad * norm_gain
    projected = jnp.mean(scaled * normin, axis=1, keepdims=True)
    normin_grad = inverse * (scaled - normin * inverse * inverse * projected)
    return (losses, normin_grad, vocab_grad)


def solution(mesh):
    torus = Mesh(mesh.devices.reshape(8, 2, 2, 4, 2), ("z", "xp", "xm", "y", "c"))
    everyone = DP + VP
    in_specs = (P(everyone, None), P(), P(None, VP), P(VP), P(DP))
    out_specs = (P(everyone), P(everyone, None), P(DP, VP))

    return jax.shard_map(
        per_device, mesh=torus, in_specs=in_specs, out_specs=out_specs, check_vma=False
    )
```
